32 devices in a mesh: sp: 8 (over z, x), tp: 4 (over y, core).
Axes of the slice: x: 2, y: 2, z: 4, core: 2. Of those that a mesh axis runs over, the one named last changes fastest.
Arguments:
- pool_input: bfloat16 [2048, 256], P('sp', 'tp'), may hold values from -6 to 6
- pool_weight: bfloat16 [4, 64, 64], P('tp'), may hold values from -0.75 to 0.75
- pool_gain: bfloat16 [256], P('tp'), may hold values from 0.099609375 to 1.8984375
- out_weight: bfloat16 [256, 2048], P(None, 'tp'), may hold values from -0.375 to 0.375
- resid: bfloat16 [2048, 2048], P('sp', 'tp'), may hold values from -90 to 90
- norm_gain: bfloat16 [2048], P('tp'), may hold values from 0.099609375 to 1.8984375
- routes: int32 [2048, 2], P('sp'), may hold values from 0 to 7, all different within a row; in each aligned block of 256 rows (0 to 255, 256 to 511, ...) at most 128 rows name the same one
- route_weight: float32 [2048, 2], P('sp'), may hold values from 0.2 to 1
- expert_gate: bfloat16 [8, 2048, 4096], P('sp', None, 'tp'), may hold values from -0.375 to 0.375
- expert_up: bfloat16 [8, 2048, 4096], P('sp', None, 'tp'), may hold values from -0.375 to 0.375
- expert_down: bfloat16 [8, 4096, 2048], P('sp', 'tp'), may hold values from -0.0234375 to 0.0234375
Outputs:
- layer_out: bfloat16 [2048, 2048], P('sp', 'tp')
The draws below stay inside these ranges and needn't reach their ends.
Inputs may be any that keep to these rules, and one draw needn't show every extreme that they name: `routes`: the 2 experts of a position differ. In each aligned block of 256 positions no expert is named by more than 128 assignments; some block reaches that bound.
All inputs are finite; a program needn't handle non-finite values.
Results may differ from the reference program's by a relative error of at most 0.0085.
Values may be sent and summed in bfloat16 or wider, within the bound.
A program may use at most 64 MiB of HBM per device.

```python
import math
from functools import partial
import jax
import jax.numpy as jnp
import numpy as np
from jax import lax

D = 2048
FF = 4096
GSIZE = 64
REACH = 16
TOPK = 2
TOK_SP = 256
GROUPS = 4
PW = 256
EXPERTS = 8
CAP = 128
TOKENS = 2048
N_SP = 8
N_TP = 4


def draw_resid(key, part):
    key_jitter, key_rows = jax.random.split(key, 2)
    column = 0.3 * 10.0 ** (jnp.arange(D, dtype=jnp.float32) / D)
    jitter = jnp.clip(jax.random.normal(key_jitter, (TOKENS, D), jnp.float32), -6.0, 6.0)
    spread = jax.random.uniform(key_rows, (TOKENS, 1), jnp.float32, 0.0, 0.5)
    return (jitter * column * 10.0 ** spread).astype(jnp.bfloat16)


def spiked(values, stream_key, source, target, parts, factor):
    def block_of(dim):
        return (jnp.arange(values.shape[dim]) // (values.shape[dim] // parts)).reshape((-1,) + (1,) * (values.ndim - 1 - dim))

    near = jax.random.permutation(stream_key, parts)[block_of(target)]
    other_side = (block_of(target) + parts // 2) % parts
    return jnp.where((block_of(source) == near) | (block_of(source) == other_side), factor * values, values)


def block_levels(key, shape, pieces, smallest, largest):
    gain, own = 1.0, jax.random.fold_in(key, 6)
    for dim, shards_of in pieces:
        draws = jnp.exp(jax.random.uniform(jax.random.fold_in(own, dim), (shards_of,), jnp.float32, smallest / len(pieces), largest / len(pieces)))
        gain = gain * jnp.repeat(draws, shape[dim] // shards_of).reshape([-1 if axis == dim else 1 for axis in range(len(shape))])
    return gain


def routed_block(own_key, own, number, rows, amount, top, bound, slope):
    sequence = jax.random.permutation(own_key, amount)
    crowded, usual = shares(amount, rows * top, bound, slope, True), shares(amount, rows * top, bound, slope, False)
    places = jnp.arange(amount)

    def named(lengths, turn):
        used = int((lengths > 0).sum())
        fixed = max(1, used // 4)
        passed = fixed + (places - fixed + turn * (used - fixed)) % max(1, amount - fixed)
        return jnp.zeros((amount,), jnp.int32).at[sequence[jnp.where(places < fixed, places, passed)]].set(jnp.asarray(lengths, jnp.int32))

    lengths = jnp.where(number % 4 == 0, named(crowded, number // 4), named(usual, number - number // 4 - 1))
    mixed = jax.random.permutation(jax.random.fold_in(own, 3), amount)
    donor, receiver = mixed[0:amount // 2 * 2:2], mixed[1:amount // 2 * 2:2]
    margin = jnp.minimum(lengths[donor] - 1, bound - lengths[receiver]) // 2
    margin = jnp.where((donor == sequence[0]) | (receiver == sequence[0]) | (lengths[receiver] == 0), 0, jnp.maximum(margin, 0))
    passed = jax.random.randint(jax.random.fold_in(own, 4), (amount // 2,), 0, 1 << 20) % (margin + 1)
    lengths = lengths.at[donor].add(-passed).at[receiver].add(passed)
    items = jnp.searchsorted(jnp.cumsum(lengths), jnp.arange(rows * top), side="right").astype(jnp.int32)
    listing = items.reshape(top, rows).T
    listing = listing[jax.random.permutation(jax.random.fold_in(own, 1), rows)]
    turn = jax.random.randint(jax.random.fold_in(own, 2), (rows, 1), 0, top)
    return jnp.take_along_axis(listing, (jnp.arange(top)[None, :] + turn) % top, axis=1)


def shares(amount, total, bound, skew, full):
    weights = [(1 << 20) // math.isqrt(rank ** skew) + 1 for rank in range(1, amount + 1)]
    largest = bound if full else min(bound, max(-(-total // amount), total * weights[0] // sum(weights)))
    least = 1 if total - largest >= amount - 1 else 0
    holding, surplus = [largest] + [least] * (amount - 1), total - largest - least * (amount - 1)
    while surplus > 0:
        movable = [i for i in range(1, amount) if holding[i] < largest] or [i for i in range(1, amount) if holding[i] < bound]
        mass, remaining = sum([weights[i] for i in movable]), surplus
        for i in movable:
            more = min(bound - holding[i], max(1, remaining * weights[i] // mass), surplus)
            holding[i] = holding[i] + more
            surplus = surplus - more
    return np.array(holding)


def bell_draw(key, shape, scale, limit, pieces=(), kind=jnp.bfloat16):
    factor_of = block_levels(key, shape, pieces, -0.22, 0.18) if pieces else 1.0
    entries = jax.random.normal(key, shape, jnp.float32) * scale * factor_of
    return jnp.minimum(jnp.maximum(entries, -limit), limit).astype(kind)


def heavy_noise(own_key, extent, scale, most, cuts, heavy, held_as=jnp.bfloat16):
    entries = scale * jax.random.normal(own_key, extent, jnp.float32)
    if cuts:
        entries = entries * block_levels(own_key, extent, cuts, -0.22, 0.18)
    return jnp.clip(spiked(entries, jax.random.fold_in(own_key, 3), *heavy), -most, most).astype(held_as)


def setup_inputs(seed: int = 0) -> dict:
    arg_keys = jax.random.split(jax.random.key(seed), 12)
    pool_input = bell_draw(arg_keys[0], (TOKENS, PW), 1.0, 6.0, ((0, 8), (1, 4)))
    pool_weight = bell_draw(arg_keys[1], (GROUPS, GSIZE, GSIZE), GSIZE ** -0.5, 0.75, ((0, 4),))
    pool_gain = jnp.clip(1.0 + 0.18 * jax.random.normal(arg_keys[2], (PW,), jnp.float32), 0.099609375, 1.8984375).astype(jnp.bfloat16)
    out_weight = bell_draw(arg_keys[3], (PW, D), PW ** -0.5, 0.375, ((1, 4),))
    resid = draw_resid(jax.random.fold_in(arg_keys[11], 71), 0)
    norm_gain = jnp.clip(1.0 + 0.18 * jax.random.normal(arg_keys[5], (D,), jnp.float32), 0.099609375, 1.8984375).astype(jnp.bfloat16)
    routes_keys = jax.random.split(jax.random.fold_in(arg_keys[6], 1), TOKENS // TOK_SP)
    routes_turns = jax.random.permutation(jax.random.fold_in(arg_keys[6], 3), TOKENS // TOK_SP)
    routes = jax.vmap(lambda own, number: routed_block(jax.random.fold_in(arg_keys[6], 2), own, number, TOK_SP, EXPERTS, TOPK, CAP, 1))(routes_keys, routes_turns).reshape((TOKENS, TOPK))
    route_weight = jnp.clip(0.2 + 0.8 * jax.random.uniform(arg_keys[7], (TOKENS, TOPK), jnp.float32) ** block_levels(arg_keys[7], (TOKENS, TOPK), ((0, 8),), -0.2, 0.2), 0.2, 1.0)
    expert_gate = bell_draw(arg_keys[8], (EXPERTS, D, FF), (D // 9) ** -0.5, 0.375, ((0, 8), (2, 4)))
    expert_up = bell_draw(arg_keys[9], (EXPERTS, D, FF), (D // 9) ** -0.5, 0.375, ((0, 8), (2, 4)))
    expert_down = heavy_noise(arg_keys[10], (EXPERTS, FF, D), (FF * 32) ** -0.5, 0.0234375, ((0, 8), (1, 4)), (1, 2, 4, 2.0))
    return {"pool_input": pool_input, "pool_weight": pool_weight, "pool_gain": pool_gain, "out_weight": out_weight, "resid": resid, "norm_gain": norm_gain, "routes": routes, "route_weight": route_weight, "expert_gate": expert_gate, "expert_up": expert_up, "expert_down": expert_down}


GATE_LIMIT = 7.0
GATE_ALPHA = 1.702
NORM_EPS = 1e-05

def clamped_unit(gate_pre, up_pre):
    gate_cut = jnp.minimum(gate_pre, GATE_LIMIT)
    up_cut = jnp.clip(up_pre, -GATE_LIMIT, GATE_LIMIT)
    return (up_cut + 1.0) * gate_cut * jax.nn.sigmoid(GATE_ALPHA * gate_cut)

def window_pool(extended, width_of, position, tok_count):
    summed = jnp.zeros((tok_count, extended.shape[1]), jnp.float32)
    for offset in range(REACH):
        first_row = REACH - 1 - offset
        shifted = extended[first_row:first_row + tok_count]
        summed = summed + jnp.where(offset < width_of[None, :], shifted, 0.0)
    counted = jnp.minimum(position[:, None] + 1, width_of[None, :]).astype(jnp.float32)
    current = extended[REACH - 1:]
    return (summed / counted - current).astype(jnp.bfloat16)

def slot_of(route_block, expert_count, capacity):
    flattened = route_block.reshape(-1).astype(jnp.int32)
    onehot = (flattened[:, None] == jnp.arange(expert_count, dtype=jnp.int32)[None, :]).astype(jnp.int32)
    earlier = (jnp.cumsum(onehot, axis=0) - onehot).astype(jnp.int32)
    ranked = lax.optimization_barrier(jnp.sum(earlier * onehot, axis=1)).astype(jnp.int32)
    return (flattened * capacity + ranked).astype(jnp.int32)

def fill_table(slot_row, id_row, weight_row):
    id_table = jnp.full((EXPERTS * CAP,), TOKENS, jnp.int32).at[slot_row].set(id_row)
    weight_table = jnp.zeros((EXPERTS * CAP,), jnp.float32).at[slot_row].set(weight_row)
    return (id_table, weight_table)

def reference(pool_input, pool_weight, pool_gain, out_weight, resid, norm_gain, routes, route_weight, expert_gate, expert_up, expert_down):
    channels = pool_input.shape[1]
    width_of = 2 ** (1 + jnp.arange(channels, dtype=jnp.int32) // GSIZE % 4)
    position = jnp.arange(TOKENS, dtype=jnp.int32)
    extended = jnp.concatenate([jnp.zeros((REACH - 1, channels), jnp.float32), pool_input.astype(jnp.float32)], axis=0)
    pooled = window_pool(extended, width_of, position, TOKENS)
    grouped = jnp.einsum('tgc,gcd->tgd', pooled.reshape(TOKENS, GROUPS, GSIZE).astype(jnp.float32), pool_weight.astype(jnp.float32))
    mixed_out = (grouped * pool_gain.astype(jnp.float32).reshape(GROUPS, GSIZE)).astype(jnp.bfloat16).reshape(TOKENS, PW)
    projected = jnp.dot(mixed_out, out_weight, preferred_element_type=jnp.float32)
    stored = lax.optimization_barrier((resid.astype(jnp.float32) + projected).astype(jnp.bfloat16))
    stream = stored.astype(jnp.float32)
    scale_row = lax.rsqrt(lax.optimization_barrier(jnp.mean(stream * stream, axis=1, keepdims=True)) + NORM_EPS)
    normed = (stream * scale_row * norm_gain.astype(jnp.float32)).astype(jnp.bfloat16)
    slots = jax.vmap(partial(slot_of, expert_count=EXPERTS, capacity=CAP))(routes.reshape(N_SP, TOK_SP, TOPK))
    token_ids = jnp.repeat(jnp.arange(TOKENS, dtype=jnp.int32), TOPK).reshape(N_SP, TOK_SP * TOPK)
    weights = route_weight.astype(jnp.float32).reshape(N_SP, TOK_SP * TOPK)
    id_tables, weight_tables = jax.vmap(fill_table)(slots, token_ids, weights)
    id_tables = id_tables.reshape(N_SP, EXPERTS, CAP).transpose(1, 0, 2).reshape(EXPERTS, N_SP * CAP)
    weight_tables = weight_tables.reshape(N_SP, EXPERTS, CAP).transpose(1, 0, 2).reshape(EXPERTS, N_SP * CAP)
    hidden_part = FF // N_TP

    def expert_step(running, inputs):
        id_row, weight_row, gate_w, up_w, down_w = inputs
        chosen = jnp.take(normed, id_row, axis=0, mode='fill', fill_value=0)
        gate_pre = jnp.dot(chosen, gate_w, preferred_element_type=jnp.float32)
        up_pre = jnp.dot(chosen, up_w, preferred_element_type=jnp.float32)
        hidden = clamped_unit(gate_pre, up_pre).astype(jnp.bfloat16)
        summed = jnp.zeros((id_row.shape[0], D), jnp.float32)
        for block_idx in range(N_TP):
            lower = block_idx * hidden_part
            partial_out = jnp.dot(hidden[:, lower:lower + hidden_part], down_w[lower:lower + hidden_part], preferred_element_type=jnp.float32)
            rounded = lax.optimization_barrier(partial_out.astype(jnp.bfloat16))
            summed = summed + rounded.astype(jnp.float32)
        output_rows = lax.optimization_barrier(summed.astype(jnp.bfloat16)).astype(jnp.float32)
        running = running.at[id_row].add(output_rows * weight_row[:, None], mode='drop')
        return (running, None)
    running, ignored = lax.scan(expert_step, jnp.zeros((TOKENS, D), jnp.float32), (id_tables, weight_tables, expert_gate, expert_up, expert_down))
    return (stream + running).astype(jnp.bfloat16)
```

```python
import functools

import jax
import jax.numpy as jnp
from jax import lax
from jax.experimental import pallas as pl
from jax.experimental.pallas import tpu as pltpu
from jax.sharding import PartitionSpec as P

GSIZE = 64
REACH = 16
TOPK = 2
CORES = 2
LANES = 128
CHUNK_ROWS = 256

GATE_LIMIT = 7.0
GATE_ALPHA = 1.702
NORM_EPS = 1e-05

F32 = jnp.float32
BF16 = jnp.bfloat16
MESH = pl.DeviceIdType.MESH


def from_behind(value, axis, steps):
    count = lax.axis_size(axis)
    first, last = (max(0, -steps), min(count, count - steps))
    return lax.ppermute(value, axis, [(source, source + steps) for source in range(first, last)])


def window_pool(extended, width_of, position, tok_count):
    summed = jnp.zeros((tok_count, extended.shape[1]), F32)
    for offset in range(REACH):
        first_row = REACH - 1 - offset
        shifted = extended[first_row : first_row + tok_count]
        summed = summed + jnp.where(offset < width_of[None, :], shifted, 0.0)
    counted = jnp.minimum(position[:, None] + 1, width_of[None, :]).astype(F32)
    current = extended[REACH - 1 :]
    return (summed / counted - current).astype(BF16)


def dot(a, b):
    return jnp.dot(a, b, preferred_element_type=F32)


def moe_kernel(
    n, tp, cap,
    stream_ref, normed_ref, routes_ref, weight_ref, gate_hbm, up_hbm, down_hbm,
    out_ref,
    x, sent, wg, wu, wd, hidden, own, mine, pc_send, pc_recv, ys_send, ys_recv, res, ret, acc,
    w_sem, a_send, a_recv, b_send, b_recv, c_send, c_recv, d_send, d_recv, e_send, e_recv, f_send, f_recv,
):
    ny = tp // CORES
    tok, feat = normed_ref.shape
    width = wg.shape[1]
    group = x.shape[0] // ys_send.shape[0]
    chunks = n // group
    rows = group * cap
    sp = lax.axis_index("sp")
    t = lax.axis_index("tp")
    y, core = t // CORES, t % CORES
    partner = y * CORES + (1 - core)

    loads = [
        pltpu.make_async_copy(gate_hbm.at[0], wg, w_sem.at[0]),
        pltpu.make_async_copy(up_hbm.at[0], wu, w_sem.at[1]),
        pltpu.make_async_copy(down_hbm.at[0], wd, w_sem.at[2]),
    ]
    for load in loads:
        load.start()

    barrier = pltpu.get_barrier_semaphore()
    peers = [(lax.rem(sp + d, n), t) for d in range(1, n)]
    peers += [(sp, lax.rem(y + k, ny) * CORES + core) for k in range(1, ny)]
    peers += [(sp, partner)]
    for peer in peers:
        pl.semaphore_signal(barrier, inc=1, device_id=peer, device_id_type=MESH)

    def cols(block):
        return pl.ds(pl.multiple_of(block * feat, LANES), feat)

    def remote(src, dst, send, recv, device):
        return pltpu.make_async_remote_copy(
            src_ref=src, dst_ref=dst, send_sem=send, recv_sem=recv, device_id=device, device_id_type=MESH
        )

    def copy_a(d):
        return remote(sent.at[d], x.at[d, :, cols(t)], a_send.at[d], a_recv.at[d], (lax.rem(sp + d, n), t))

    def copy_b(d, k):
        part = x.at[d, :, cols(t)]
        return remote(part, part, b_send.at[d, k], b_recv.at[d, k], (sp, lax.rem(y + k, ny) * CORES + core))

    def copy_c(d, k):
        part = x.at[d, :, cols(lax.rem(y + ny - k, ny) * CORES + core)]
        return remote(part, part, c_send.at[d, k], c_recv.at[d, k], (sp, partner))

    def copy_d(q):
        return remote(pc_send.at[q], pc_recv.at[q], d_send.at[q], d_recv.at[q], (sp, partner))

    def copy_e(q, k):
        return remote(
            ys_send.at[q, k], ys_recv.at[q, k], e_send.at[q, k], e_recv.at[q, k],
            (sp, lax.rem(y + k, ny) * CORES + core),
        )

    def copy_f(d):
        return remote(res.at[d], ret.at[d], f_send.at[d], f_recv.at[d], (lax.rem(sp + n - d, n), t))

    lane = lax.broadcasted_iota(jnp.int32, (tok, LANES), 1)
    routes = [routes_ref[:, k : k + 1] for k in range(TOPK)]
    onehot = [jnp.where(route == lane, 1.0, 0.0) for route in routes]
    below = lax.broadcasted_iota(jnp.int32, (tok, tok), 1) < lax.broadcasted_iota(jnp.int32, (tok, tok), 0)
    earlier = dot(jnp.where(below, 1.0, 0.0).astype(BF16), sum(onehot).astype(BF16))
    keys = [
        routes[k] * cap + jnp.sum(earlier * onehot[k], axis=1, keepdims=True).astype(jnp.int32)
        for k in range(TOPK)
    ]
    slot = lax.broadcasted_iota(jnp.int32, (tok, cap), 1)

    def rows_for(expert):
        wanted = slot + expert * cap
        chosen = jnp.where(keys[0] == wanted, 1.0, 0.0)
        for key in keys[1:]:
            chosen = chosen + jnp.where(key == wanted, 1.0, 0.0)
        return lax.dot_general(
            chosen.astype(BF16), normed_ref[...], (((0,), (0,)), ((), ())), preferred_element_type=F32
        ).astype(BF16)

    for d in range(1, n):
        sent[d] = rows_for(lax.rem(sp + d, n))
        if d == 1:
            pl.semaphore_wait(barrier, len(peers))
        copy_a(d).start()
    x[0, :, cols(t)] = rows_for(sp)

    def forward_a(q):
        for d in range(q * group, (q + 1) * group):
            if d:
                copy_a(d).wait_recv()
            for k in range(1, ny):
                copy_b(d, k).start()
            copy_c(d, 0).start()

    def finish(q):
        total = mine[q]
        for k in range(1, ny):
            copy_e(q, k).wait_recv()
            total = total + ys_recv[q, k].astype(F32)
        total = total.astype(BF16)
        for i in range(group):
            d = q * group + i
            block = total[i * cap : (i + 1) * cap]
            if d:
                res[d] = block
                copy_f(d).start()
            else:
                ret[0] = block

    forward_a(0)
    for q in range(chunks):
        members = range(q * group, (q + 1) * group)
        if q + 1 < chunks:
            forward_a(q + 1)
        for d in members:
            for k in range(1, ny):
                copy_b(d, k).wait_recv()
                copy_c(d, k).start()
        for d in members:
            for k in range(ny):
                copy_c(d, k).wait_recv()
        if q == 0:
            loads[0].wait()
            loads[1].wait()

        step = min(width, 256)

        @pl.loop(0, width // step)
        def _(i):
            part = pl.ds(pl.multiple_of(i * step, LANES), step)
            chosen = x[q * group : (q + 1) * group].reshape(rows, x.shape[2])
            gate = jnp.minimum(dot(chosen, wg[:, part]), GATE_LIMIT)
            up = jnp.clip(dot(chosen, wu[:, part]), -GATE_LIMIT, GATE_LIMIT)
            hidden[:, part] = ((up + 1.0) * gate * jax.nn.sigmoid(GATE_ALPHA * gate)).astype(BF16)

        if q == 0:
            loads[2].wait()
        for k in range(ny):
            block = lax.rem(y + k, ny) * CORES + (1 - core)
            pc_send[q, :, k * feat : (k + 1) * feat] = dot(hidden[...], wd[:, cols(block)]).astype(BF16)
        copy_d(q).start()
        for k in range(ny):
            block = lax.rem(y + k, ny) * CORES + core
            own[:, k * feat : (k + 1) * feat] = dot(hidden[...], wd[:, cols(block)])
        if q:
            finish(q - 1)
        copy_d(q).wait_recv()
        for k in range(1, ny):
            part = slice(k * feat, (k + 1) * feat)
            ys_send[q, k] = (own[:, part] + pc_recv[q, :, part].astype(F32)).astype(BF16)
            copy_e(q, k).start()
        mine[q] = own[:, :feat] + pc_recv[q, :, :feat].astype(F32)
    finish(chunks - 1)

    heads = [weight_ref[:, k : k + 1].astype(BF16).astype(F32) for k in range(TOPK)]
    rests = [weight_ref[:, k : k + 1] - heads[k] for k in range(TOPK)]
    acc[...] = stream_ref[...].astype(F32)
    for d in range(n):
        if d:
            copy_f(d).wait_recv()
        wanted = slot + lax.rem(sp + d, n) * cap
        high = sum(jnp.where(keys[k] == wanted, heads[k], 0.0) for k in range(TOPK))
        low = sum(jnp.where(keys[k] == wanted, rests[k], 0.0) for k in range(TOPK))
        block = ret[d]
        acc[...] += dot(high.astype(BF16), block) + dot(low.astype(BF16), block)
    out_ref[...] = acc[...].astype(BF16)

    for d in range(n):
        if d:
            copy_a(d).wait_send()
            copy_f(d).wait_send()
        for k in range(ny):
            if k:
                copy_b(d, k).wait_send()
            copy_c(d, k).wait_send()
    for q in range(chunks):
        copy_d(q).wait_send()
        for k in range(1, ny):
            copy_e(q, k).wait_send()


def moe(stream, normed, routes, route_weight, expert_gate, expert_up, expert_down):
    n, tp = lax.axis_size("sp"), lax.axis_size("tp")
    tok, feat = normed.shape
    model, width = expert_gate.shape[1:]
    cap = 2 * tok * TOPK // n
    ny = tp // CORES
    group = min(n, max(1, CHUNK_ROWS // cap))
    chunks = n // group
    rows = group * cap
    sems = pltpu.SemaphoreType.DMA
    vmem = pl.BlockSpec(memory_space=pltpu.VMEM)
    hbm = pl.BlockSpec(memory_space=pl.ANY)
    return pl.pallas_call(
        functools.partial(moe_kernel, n, tp, cap),
        out_shape=jax.ShapeDtypeStruct((tok, feat), BF16),
        in_specs=[vmem] * 4 + [hbm] * 3,
        out_specs=vmem,
        scratch_shapes=[
            pltpu.VMEM((n, cap, model), BF16),
            pltpu.VMEM((n, cap, feat), BF16),
            pltpu.VMEM((model, width), BF16),
            pltpu.VMEM((model, width), BF16),
            pltpu.VMEM((width, model), BF16),
            pltpu.VMEM((rows, width), BF16),
            pltpu.VMEM((rows, ny * feat), F32),
            pltpu.VMEM((chunks, rows, feat), F32),
            pltpu.VMEM((chunks, rows, ny * feat), BF16),
            pltpu.VMEM((chunks, rows, ny * feat), BF16),
            pltpu.VMEM((chunks, ny, rows, feat), BF16),
            pltpu.VMEM((chunks, ny, rows, feat), BF16),
            pltpu.VMEM((n, cap, feat), BF16),
            pltpu.VMEM((n, cap, feat), BF16),
            pltpu.VMEM((tok, feat), F32),
            sems((3,)),
            sems((n,)), sems((n,)),
            sems((n, ny)), sems((n, ny)),
            sems((n, ny)), sems((n, ny)),
            sems((chunks,)), sems((chunks,)),
            sems((chunks, ny)), sems((chunks, ny)),
            sems((n,)), sems((n,)),
        ],
        compiler_params=pltpu.CompilerParams(
            collective_id=0, has_side_effects=True, vmem_limit_bytes=56 * 1024 * 1024
        ),
    )(stream, normed, routes, route_weight, expert_gate, expert_up, expert_down)


def on_device(
    pool_input, pool_weight, pool_gain, out_weight, resid, norm_gain,
    routes, route_weight, expert_gate, expert_up, expert_down,
):
    tok_rows, channels = pool_input.shape
    groups = pool_weight.shape[0]
    model = expert_gate.shape[1]
    tail_rows = pool_input[tok_rows - (REACH - 1) :]
    before = from_behind(tail_rows, "sp", 1)
    extended = jnp.concatenate([before, pool_input], axis=0).astype(F32)
    first_group = lax.axis_index("tp") * groups
    width_of = 2 ** (1 + (first_group + jnp.arange(channels, dtype=jnp.int32) // GSIZE) % 4)
    position = lax.axis_index("sp") * tok_rows + jnp.arange(tok_rows, dtype=jnp.int32)
    pooled = window_pool(extended, width_of, position, tok_rows)
    grouped = jnp.einsum(
        "tgc,gcd->tgd",
        pooled.reshape(tok_rows, groups, GSIZE),
        pool_weight,
        preferred_element_type=F32,
    )
    mixed_out = (
        (grouped * pool_gain.astype(F32).reshape(groups, GSIZE)).astype(BF16).reshape(tok_rows, channels)
    )
    projected = dot(lax.all_gather(mixed_out, "tp", axis=1, tiled=True), out_weight)
    stored = lax.optimization_barrier((resid.astype(F32) + projected).astype(BF16))
    stream = stored.astype(F32)
    squares = lax.psum(jnp.sum(stream * stream, axis=1), "tp")
    scale_row = lax.rsqrt(squares / model + NORM_EPS)
    normed = (stream * scale_row[:, None] * norm_gain.astype(F32)).astype(BF16)
    return moe(stored, normed, routes, route_weight, expert_gate, expert_up, expert_down)


def solution(mesh):
    in_specs = (
        P("sp", "tp"),
        P("tp", None, None),
        P("tp"),
        P(None, "tp"),
        P("sp", "tp"),
        P("tp"),
        P("sp", None),
        P("sp", None),
        P("sp", None, "tp"),
        P("sp", None, "tp"),
        P("sp", "tp", None),
    )
    return jax.shard_map(on_device, mesh=mesh, in_specs=in_specs, out_specs=P("sp", "tp"), check_vma=False)
```

```python
import functools

import jax
import jax.numpy as jnp
from jax import lax
from jax.experimental import pallas as pl
from jax.experimental.pallas import tpu as pltpu
from jax.sharding import PartitionSpec as P

GSIZE = 64
REACH = 16
TOPK = 2
CORES = 2
LANES = 128
CHUNK_ROWS = 256

GATE_LIMIT = 7.0
GATE_ALPHA = 1.702
NORM_EPS = 1e-05

F32 = jnp.float32
BF16 = jnp.bfloat16
MESH = pl.DeviceIdType.MESH


def dot(a, b):
    return jnp.dot(a, b, preferred_element_type=F32)


def layer_kernel(
    n, tp, cap,
    pool_ref, mix_ref, gain_ref, proj_ref, resid_ref, norm_ref, routes_ref, weight_ref, gate_hbm, up_hbm, down_hbm,
    out_ref,
    tail, halo, packed, squares, stream_ref, normed_ref,
    x, sent, wg, wu, wd, hidden, own, mine, pc_send, pc_recv, ys_send, ys_recv, res, ret, acc,
    w_sem, h_send, h_recv, m_send, m_recv, s_send, s_recv, a_send, a_recv, b_send, b_recv, c_send, c_recv, d_send, d_recv, e_send, e_recv, f_send, f_recv,
):
    ny = tp // CORES
    tok, feat = resid_ref.shape
    channels = pool_ref.shape[1]
    width = wg.shape[1]
    group = x.shape[0] // ys_send.shape[0]
    chunks = n // group
    rows = group * cap
    sp = lax.axis_index("sp")
    t = lax.axis_index("tp")
    y, core = t // CORES, t % CORES
    partner = y * CORES + (1 - core)

    loads = [
        pltpu.make_async_copy(gate_hbm.at[0], wg, w_sem.at[0]),
        pltpu.make_async_copy(up_hbm.at[0], wu, w_sem.at[1]),
        pltpu.make_async_copy(down_hbm.at[0], wd, w_sem.at[2]),
    ]
    for load in loads:
        load.start()

    barrier = pltpu.get_barrier_semaphore()
    peers = [(lax.rem(sp + d, n), t) for d in range(1, n)]
    peers += [(sp, lax.rem(t + k, tp)) for k in range(1, tp)]
    for peer in peers:
        pl.semaphore_signal(barrier, inc=1, device_id=peer, device_id_type=MESH)

    def cols(block):
        return pl.ds(pl.multiple_of(block * feat, LANES), feat)

    def remote(src, dst, send, recv, device):
        return pltpu.make_async_remote_copy(
            src_ref=src, dst_ref=dst, send_sem=send, recv_sem=recv, device_id=device, device_id_type=MESH
        )

    def copy_a(d):
        return remote(sent.at[d], x.at[d, :, cols(t)], a_send.at[d], a_recv.at[d], (lax.rem(sp + d, n), t))

    def copy_b(d, k):
        part = x.at[d, :, cols(t)]
        return remote(part, part, b_send.at[d, k], b_recv.at[d, k], (sp, lax.rem(y + k, ny) * CORES + core))

    def copy_c(d, k):
        part = x.at[d, :, cols(lax.rem(y + ny - k, ny) * CORES + core)]
        return remote(part, part, c_send.at[d, k], c_recv.at[d, k], (sp, partner))

    def copy_d(q):
        return remote(pc_send.at[q], pc_recv.at[q], d_send.at[q], d_recv.at[q], (sp, partner))

    def copy_e(q, k):
        return remote(
            ys_send.at[q, k], ys_recv.at[q, k], e_send.at[q, k], e_recv.at[q, k],
            (sp, lax.rem(y + k, ny) * CORES + core),
        )

    def copy_f(d):
        return remote(res.at[d], ret.at[d], f_send.at[d], f_recv.at[d], (lax.rem(sp + n - d, n), t))

    tail_copy = remote(tail, halo, h_send.at[0], h_recv.at[0], (lax.rem(sp + 1, n), t))

    def copy_m(k):
        return remote(packed.at[0], packed.at[k], m_send.at[k], m_recv.at[k], (sp, lax.rem(t + k, tp)))

    def copy_s(k):
        return remote(squares.at[0], squares.at[k], s_send.at[k], s_recv.at[k], (sp, lax.rem(t + k, tp)))

    tail[...] = jnp.zeros_like(tail)
    tail[:, :channels] = pool_ref[tok - REACH :, :].astype(F32)
    pl.semaphore_wait(barrier, len(peers))
    tail_copy.start()

    listed = jnp.concatenate(
        [routes_ref[...].astype(F32), weight_ref[...], jnp.zeros((8 - 2 * TOPK, tok), F32)], axis=0
    ).T
    routes = [listed[:, k : k + 1] for k in range(TOPK)]
    weights = [listed[:, TOPK + k : TOPK + k + 1] for k in range(TOPK)]
    lane = lax.broadcasted_iota(jnp.int32, (tok, LANES), 1).astype(F32)
    onehot = [jnp.where(route == lane, 1.0, 0.0) for route in routes]
    below = lax.broadcasted_iota(jnp.int32, (tok, tok), 1) < lax.broadcasted_iota(jnp.int32, (tok, tok), 0)
    earlier = dot(jnp.where(below, 1.0, 0.0).astype(BF16), sum(onehot).astype(BF16))
    keys = [
        routes[k] * float(cap) + jnp.sum(earlier * onehot[k], axis=1, keepdims=True) for k in range(TOPK)
    ]
    slot = lax.broadcasted_iota(jnp.int32, (tok, cap), 1)

    tail_copy.wait_recv()
    before = jnp.where(sp == 0, 0.0, halo[:, :channels])
    current = pool_ref[...].astype(F32)
    summed = jnp.concatenate([before, current], axis=0)
    groups = channels // GSIZE
    group_of = t * groups + lax.broadcasted_iota(jnp.int32, (1, channels), 1) // GSIZE
    level = lax.rem(group_of, 4)
    window, span = jnp.zeros((tok, channels), F32), jnp.zeros((1, channels), F32)
    for power in range(4):
        summed = summed + pltpu.roll(summed, 1 << power, 0)
        window = jnp.where(level == power, summed[REACH:], window)
        span = jnp.where(level == power, float(2 << power), span)
    place = (sp * tok + 1 + lax.broadcasted_iota(jnp.int32, (tok, channels), 0)).astype(F32)
    pooled = (window / jnp.minimum(place, span) - current).astype(BF16)
    mixed = jnp.concatenate(
        [dot(pooled[:, g * GSIZE : (g + 1) * GSIZE], mix_ref[g]) for g in range(groups)], axis=1
    )
    mixed = (mixed * gain_ref[...].astype(F32)).astype(BF16)
    folds = max(1, LANES // channels)
    short = tok // folds
    packed[0] = jnp.concatenate([mixed[i * short : (i + 1) * short] for i in range(folds)], axis=1)
    for k in range(1, tp):
        copy_m(k).start()

    def projected(k):
        block = packed[k]
        part = jnp.concatenate([block[:, i * channels : (i + 1) * channels] for i in range(folds)], axis=0)
        first = lax.rem(t + tp - k, tp) * channels
        return dot(part, proj_ref[pl.ds(pl.multiple_of(first, GSIZE), channels), :])

    acc[...] = resid_ref[...].astype(F32) + projected(0)
    for k in range(1, tp):
        copy_m(k).wait_recv()
        acc[...] += projected(k)
    stream_ref[...] = acc[...].astype(BF16)
    stream = stream_ref[...].astype(F32)
    power = jnp.sum(stream * stream, axis=1, keepdims=True)
    squares[0] = jnp.broadcast_to(power, (tok, LANES)).T[:8]
    for k in range(1, tp):
        copy_s(k).start()
    total = squares[0]
    for k in range(1, tp):
        copy_s(k).wait_recv()
        total = total + squares[k]
    scale = lax.rsqrt(total.T[:, :1] / x.shape[2] + NORM_EPS)
    normed_ref[...] = (stream_ref[...].astype(F32) * scale * norm_ref[...].astype(F32)).astype(BF16)

    def rows_for(expert):
        wanted = (slot + expert * cap).astype(F32)
        chosen = jnp.where(keys[0] == wanted, 1.0, 0.0)
        for key in keys[1:]:
            chosen = chosen + jnp.where(key == wanted, 1.0, 0.0)
        return lax.dot_general(
            chosen.astype(BF16), normed_ref[...], (((0,), (0,)), ((), ())), preferred_element_type=F32
        ).astype(BF16)

    for d in range(1, n):
        sent[d] = rows_for(lax.rem(sp + d, n))
        copy_a(d).start()
    x[0, :, cols(t)] = rows_for(sp)

    def forward_a(q):
        for d in range(q * group, (q + 1) * group):
            if d:
                copy_a(d).wait_recv()
            for k in range(1, ny):
                copy_b(d, k).start()
            copy_c(d, 0).start()

    def finish(q):
        total = mine[q]
        for k in range(1, ny):
            copy_e(q, k).wait_recv()
            total = total + ys_recv[q, k].astype(F32)
        total = total.astype(BF16)
        for i in range(group):
            d = q * group + i
            block = total[i * cap : (i + 1) * cap]
            if d:
                res[d] = block
                copy_f(d).start()
            else:
                ret[0] = block

    forward_a(0)
    for q in range(chunks):
        members = range(q * group, (q + 1) * group)
        if q + 1 < chunks:
            forward_a(q + 1)
        for d in members:
            for k in range(1, ny):
                copy_b(d, k).wait_recv()
                copy_c(d, k).start()
        for d in members:
            for k in range(ny):
                copy_c(d, k).wait_recv()
        if q == 0:
            loads[0].wait()
            loads[1].wait()

        step = min(width, 256)

        @pl.loop(0, width // step)
        def _(i):
            part = pl.ds(pl.multiple_of(i * step, LANES), step)
            chosen = x[q * group : (q + 1) * group].reshape(rows, x.shape[2])
            gate = jnp.minimum(dot(chosen, wg[:, part]), GATE_LIMIT)
            up = jnp.clip(dot(chosen, wu[:, part]), -GATE_LIMIT, GATE_LIMIT)
            hidden[:, part] = ((up + 1.0) * gate * jax.nn.sigmoid(GATE_ALPHA * gate)).astype(BF16)

        if q == 0:
            loads[2].wait()
        for k in range(ny):
            block = lax.rem(y + k, ny) * CORES + (1 - core)
            pc_send[q, :, k * feat : (k + 1) * feat] = dot(hidden[...], wd[:, cols(block)]).astype(BF16)
        copy_d(q).start()
        for k in range(ny):
            block = lax.rem(y + k, ny) * CORES + core
            own[:, k * feat : (k + 1) * feat] = dot(hidden[...], wd[:, cols(block)])
        if q:
            finish(q - 1)
        copy_d(q).wait_recv()
        for k in range(1, ny):
            part = slice(k * feat, (k + 1) * feat)
            ys_send[q, k] = (own[:, part] + pc_recv[q, :, part].astype(F32)).astype(BF16)
            copy_e(q, k).start()
        mine[q] = own[:, :feat] + pc_recv[q, :, :feat].astype(F32)
    finish(chunks - 1)

    heads = [weight.astype(BF16).astype(F32) for weight in weights]
    rests = [weights[k] - heads[k] for k in range(TOPK)]
    acc[...] = stream_ref[...].astype(F32)
    for d in range(n):
        if d:
            copy_f(d).wait_recv()
        wanted = (slot + lax.rem(sp + d, n) * cap).astype(F32)
        high = sum(jnp.where(keys[k] == wanted, heads[k], 0.0) for k in range(TOPK))
        low = sum(jnp.where(keys[k] == wanted, rests[k], 0.0) for k in range(TOPK))
        block = ret[d]
        acc[...] += dot(high.astype(BF16), block) + dot(low.astype(BF16), block)
    out_ref[...] = acc[...].astype(BF16)

    tail_copy.wait_send()
    for k in range(1, tp):
        copy_m(k).wait_send()
        copy_s(k).wait_send()
    for d in range(n):
        if d:
            copy_a(d).wait_send()
            copy_f(d).wait_send()
        for k in range(ny):
            if k:
                copy_b(d, k).wait_send()
            copy_c(d, k).wait_send()
    for q in range(chunks):
        copy_d(q).wait_send()
        for k in range(1, ny):
            copy_e(q, k).wait_send()


def on_device(
    pool_input, pool_weight, pool_gain, out_weight, resid, norm_gain,
    routes, route_weight, expert_gate, expert_up, expert_down,
):
    n, tp = lax.axis_size("sp"), lax.axis_size("tp")
    tok, feat = resid.shape
    channels = pool_input.shape[1]
    folds = max(1, LANES // channels)
    model, width = expert_gate.shape[1:]
    cap = 2 * tok * TOPK // n
    ny = tp // CORES
    group = min(n, max(1, CHUNK_ROWS // cap))
    chunks = n // group
    rows = group * cap
    sems = pltpu.SemaphoreType.DMA
    vmem = pl.BlockSpec(memory_space=pltpu.VMEM)
    hbm = pl.BlockSpec(memory_space=pl.ANY)
    return pl.pallas_call(
        functools.partial(layer_kernel, n, tp, cap),
        out_shape=jax.ShapeDtypeStruct((tok, feat), BF16),
        in_specs=[vmem] * 8 + [hbm] * 3,
        out_specs=vmem,
        scratch_shapes=[
            pltpu.VMEM((REACH, max(LANES, channels)), F32),
            pltpu.VMEM((REACH, max(LANES, channels)), F32),
            pltpu.VMEM((tp, tok // folds, folds * channels), BF16),
            pltpu.VMEM((tp, 8, tok), F32),
            pltpu.VMEM((tok, feat), BF16),
            pltpu.VMEM((tok, feat), BF16),
            pltpu.VMEM((n, cap, model), BF16),
            pltpu.VMEM((n, cap, feat), BF16),
            pltpu.VMEM((model, width), BF16),
            pltpu.VMEM((model, width), BF16),
            pltpu.VMEM((width, model), BF16),
            pltpu.VMEM((rows, width), BF16),
            pltpu.VMEM((rows, ny * feat), F32),
            pltpu.VMEM((chunks, rows, feat), F32),
            pltpu.VMEM((chunks, rows, ny * feat), BF16),
            pltpu.VMEM((chunks, rows, ny * feat), BF16),
            pltpu.VMEM((chunks, ny, rows, feat), BF16),
            pltpu.VMEM((chunks, ny, rows, feat), BF16),
            pltpu.VMEM((n, cap, feat), BF16),
            pltpu.VMEM((n, cap, feat), BF16),
            pltpu.VMEM((tok, feat), F32),
            sems((3,)),
            sems((1,)), sems((1,)),
            sems((tp,)), sems((tp,)),
            sems((tp,)), sems((tp,)),
            sems((n,)), sems((n,)),
            sems((n, ny)), sems((n, ny)),
            sems((n, ny)), sems((n, ny)),
            sems((chunks,)), sems((chunks,)),
            sems((chunks, ny)), sems((chunks, ny)),
            sems((n,)), sems((n,)),
        ],
        compiler_params=pltpu.CompilerParams(
            collective_id=0, has_side_effects=True, vmem_limit_bytes=56 * 1024 * 1024
        ),
    )(
        pool_input, pool_weight, pool_gain.reshape(1, -1), out_weight, resid, norm_gain.reshape(1, -1),
        routes.T, route_weight.T, expert_gate, expert_up, expert_down,
    )


def solution(mesh):
    in_specs = (
        P("sp", "tp"),
        P("tp", None, None),
        P("tp"),
        P(None, "tp"),
        P("sp", "tp"),
        P("tp"),
        P("sp", None),
        P("sp", None),
        P("sp", None, "tp"),
        P("sp", None, "tp"),
        P("sp", "tp", None),
    )
    return jax.shard_map(on_device, mesh=mesh, in_specs=in_specs, out_specs=P("sp", "tp"), check_vma=False)
```
